32 devices in a mesh: sp: 16 (over z, y, core), tp: 2 (over x).
Axes of the slice: x: 2, y: 2, z: 4, core: 2. Of those that a mesh axis runs over, the one named last changes fastest.
Arguments:
- inputs: bfloat16 [8192, 3072], P('sp', 'tp'), may hold values from -6 to 6
- w_query: bfloat16 [3072, 1536], P(None, 'tp'), may hold values from -0.109375 to 0.109375
- w_key: bfloat16 [3072, 1536], P(None, 'tp'), may hold values from -0.109375 to 0.109375
- w_value: bfloat16 [3072, 1536], P(None, 'tp'), may hold values from -0.109375 to 0.109375
- rel_bias: float32 [320, 24], P(None, 'tp'), may hold values from -5 to 254
- d_out: bfloat16 [8192, 1536], P('sp', 'tp'), may hold values from -6 to 6
Outputs:
- grad_inputs: bfloat16 [8192, 3072], P('sp', 'tp')
- grad_w_query: float32 [3072, 1536], P('sp', 'tp')
- grad_w_key: float32 [3072, 1536], P('sp', 'tp')
- grad_w_value: float32 [3072, 1536], P('sp', 'tp')
- grad_bias: float32 [320, 24], P(None, 'tp')
The draws below stay inside these ranges and needn't reach their ends.
All inputs are finite; a program needn't handle non-finite values.
Results may differ from the reference program's by a relative error of at most 0.015.
Values may be sent and summed in bfloat16 or wider, within the bound.
No kernel may reach another device: no remote copies, remote signals or barrier semaphores. Data moves between devices by JAX's collectives and lax.ppermute only.
A program may use at most 128 MiB of HBM per device.

```python
import jax
import jax.numpy as jnp
import numpy as np
from jax import lax

D = 3072
HEADS = 24
HEAD = 64
SEG = 64
LEFT = 4
REL_MAX = 256
ATT = 1536
REL_SIZE = 320
TOKENS = 8192
N_TP = 2


def draw_rel_bias(key, part):
    base = jnp.clip(jax.random.normal(key, (REL_SIZE, HEADS), jnp.float32), -5.0, 5.0)
    return base


def spiked(drawn, rng, source, target, parts, factor):
    def block_of(position):
        return (jnp.arange(drawn.shape[position]) // (drawn.shape[position] // parts)).reshape((-1,) + (1,) * (drawn.ndim - 1 - position))

    near = jax.random.permutation(rng, parts)[block_of(target)]
    far = (block_of(target) + parts // 2) % parts
    return jnp.where((block_of(source) == near) | (block_of(source) == far), factor * drawn, drawn)


def levels(key, extent, shards, smallest, largest):
    gain = 1.0
    for axis_at, shards_of in shards:
        steps = jax.random.uniform(jax.random.fold_in(jax.random.fold_in(key, 6), axis_at), (shards_of,), jnp.float32, smallest / len(shards), largest / len(shards))
        gain = gain * jnp.repeat(jnp.exp(steps), extent[axis_at] // shards_of).reshape((-1,) + (1,) * (len(extent) - 1 - axis_at))
    return gain


def noise(own_key, dims, scale, reach, cuts=(), held_as=jnp.bfloat16):
    factor_of = levels(own_key, dims, cuts, -0.22, 0.18) if cuts else 1.0
    entries = jax.random.normal(own_key, dims, jnp.float32) * scale * factor_of
    return jnp.minimum(jnp.maximum(entries, -reach), reach).astype(held_as)


def heavy_noise(own_key, extent, scale, most, split, heavy, held_as=jnp.bfloat16):
    array = scale * jax.random.normal(own_key, extent, jnp.float32)
    if split:
        array = array * levels(own_key, extent, split, -0.22, 0.18)
    return jnp.clip(spiked(array, jax.random.fold_in(own_key, 3), *heavy), -most, most).astype(held_as)


def setup_inputs(seed: int = 0) -> dict:
    keys = jax.random.split(jax.random.key(seed), 7)
    inputs = heavy_noise(keys[0], (TOKENS, D), 1.0, 6.0, ((0, 16), (1, 2)), (0, 1, 16, 2.0))
    w_query = noise(keys[1], (D, ATT), D ** -0.5, 0.109375, ((1, 2),))
    w_key = noise(keys[2], (D, ATT), D ** -0.5, 0.109375, ((1, 2),))
    w_value = noise(keys[3], (D, ATT), D ** -0.5, 0.109375, ((1, 2),))
    rel_bias = draw_rel_bias(jax.random.fold_in(keys[6], 71), 0)
    d_out = noise(keys[5], (TOKENS, ATT), 1.0, 6.0, ((0, 16), (1, 2)))
    return dict(inputs=inputs, w_query=w_query, w_key=w_key, w_value=w_value, rel_bias=rel_bias, d_out=d_out)


def bias_table(rel_bias):
    query_row = np.arange(SEG)[:, None]
    key_row = np.arange((LEFT + 1) * SEG)[None, :]
    distance = np.clip(LEFT * SEG + query_row - key_row, 1 - SEG, REL_MAX) + SEG - 1
    picked = jnp.take(rel_bias, jnp.asarray(distance.astype(np.int32)), axis=0)
    return jnp.transpose(picked, (2, 0, 1))

def banded(source, seg_count):
    pieces = source.reshape((seg_count + LEFT, SEG) + source.shape[1:])
    return jnp.concatenate([pieces[offset_seg:offset_seg + seg_count] for offset_seg in range(LEFT + 1)], axis=1)

def unbanded(band_grads, seg_count):
    pieces = band_grads.reshape((seg_count, LEFT + 1, SEG) + band_grads.shape[2:])
    widths = ((0, 0),) * (pieces.ndim - 3)
    total = jnp.zeros((seg_count + LEFT, SEG) + band_grads.shape[2:], band_grads.dtype)
    for offset_seg in range(LEFT + 1):
        total = total + jnp.pad(pieces[:, offset_seg], ((offset_seg, LEFT - offset_seg), (0, 0)) + widths)
    return total.reshape(((seg_count + LEFT) * SEG,) + band_grads.shape[2:])

def one_head(operands):
    q_head, k_head, v_head, d_head, bias_head = operands
    seg_count = TOKENS // SEG
    score_scale = HEAD ** (-0.5)
    pad_rows = ((LEFT * SEG, 0), (0, 0))
    key_band = banded(jnp.pad(k_head, pad_rows), seg_count).astype(jnp.float32)
    value_band = banded(jnp.pad(v_head, pad_rows), seg_count).astype(jnp.float32)
    q_seg = q_head.reshape(seg_count, SEG, HEAD).astype(jnp.float32)
    d_seg = d_head.reshape(seg_count, SEG, HEAD).astype(jnp.float32)
    scores = jnp.einsum('cqd,ckd->cqk', q_seg, key_band) * score_scale + bias_head[None]
    key_pos = (jnp.arange(seg_count)[:, None] - LEFT) * SEG + jnp.arange((LEFT + 1) * SEG)[None, :]
    scores = jnp.where((key_pos >= 0)[:, None, :], scores, -jnp.inf)
    top = lax.optimization_barrier(jnp.max(scores, axis=-1, keepdims=True))
    lse = top + jnp.log(lax.optimization_barrier(jnp.sum(jnp.exp(scores - top), axis=-1, keepdims=True)))
    prob = jnp.exp(scores - lse)
    prob_low = prob.astype(jnp.bfloat16).astype(jnp.float32)
    attended = jnp.einsum('cqk,ckd->cqd', prob_low, value_band)
    delta = lax.optimization_barrier(jnp.sum(d_seg * attended, axis=-1, keepdims=True))
    grad_prob = jnp.einsum('cqd,ckd->cqk', d_seg, value_band)
    dscore = prob * (grad_prob - delta)
    dscore_low = dscore.astype(jnp.bfloat16).astype(jnp.float32)
    grad_query = jnp.einsum('cqk,ckd->cqd', dscore_low, key_band) * score_scale
    grad_kband = jnp.einsum('cqk,cqd->ckd', dscore_low, q_seg) * score_scale
    grad_vband = jnp.einsum('cqk,cqd->ckd', prob_low, d_seg)
    grad_key = unbanded(grad_kband, seg_count)[LEFT * SEG:]
    grad_value = unbanded(grad_vband, seg_count)[LEFT * SEG:]
    return (grad_query.reshape(TOKENS, HEAD).astype(jnp.bfloat16), grad_key.astype(jnp.bfloat16), grad_value.astype(jnp.bfloat16), lax.optimization_barrier(jnp.sum(dscore, axis=0)))

def reference(inputs, w_query, w_key, w_value, rel_bias, d_out):
    query = jnp.dot(inputs, w_query, preferred_element_type=jnp.float32).astype(jnp.bfloat16)
    key = jnp.dot(inputs, w_key, preferred_element_type=jnp.float32).astype(jnp.bfloat16)
    value = jnp.dot(inputs, w_value, preferred_element_type=jnp.float32).astype(jnp.bfloat16)

    def by_head(matrix):
        return matrix.reshape(TOKENS, HEADS, HEAD).transpose(1, 0, 2)

    def by_token(matrix):
        return matrix.transpose(1, 0, 2).reshape(TOKENS, HEADS * HEAD)
    bias_full, bias_back = jax.vjp(bias_table, rel_bias)
    head_q, head_k, head_v, score_sum = lax.map(one_head, (by_head(query), by_head(key), by_head(value), by_head(d_out), bias_full))
    grad_query = by_token(head_q)
    grad_key = by_token(head_k)
    grad_value = by_token(head_v)
    grad_bias = bias_back(score_sum)[0]
    contract = (((0,), (0,)), ((), ()))
    grad_w_query = lax.dot_general(inputs, grad_query, contract, preferred_element_type=jnp.float32)
    grad_w_key = lax.dot_general(inputs, grad_key, contract, preferred_element_type=jnp.float32)
    grad_w_value = lax.dot_general(inputs, grad_value, contract, preferred_element_type=jnp.float32)
    group = HEADS * HEAD // N_TP
    total = jnp.zeros((TOKENS, D), jnp.float32)
    for index in range(N_TP):
        cols = slice(index * group, (index + 1) * group)
        partial_value = jnp.dot(grad_query[:, cols], w_query[:, cols].T, preferred_element_type=jnp.float32)
        partial_value = partial_value + jnp.dot(grad_key[:, cols], w_key[:, cols].T, preferred_element_type=jnp.float32)
        partial_value = partial_value + jnp.dot(grad_value[:, cols], w_value[:, cols].T, preferred_element_type=jnp.float32)
        rounded = lax.optimization_barrier(partial_value.astype(jnp.bfloat16))
        total = total + rounded.astype(jnp.float32)
    grad_inputs = total.astype(jnp.bfloat16)
    return (grad_inputs, grad_w_query, grad_w_key, grad_w_value, grad_bias)
```

```python
import jax
import jax.numpy as jnp
from jax import lax
from jax.experimental import pallas as pl
from jax.experimental.pallas import tpu as pltpu
from jax.sharding import PartitionSpec as P

HEAD = 64
SEG = 64
LEFT = 4
REL_MAX = 256
PAIR = 2 * HEAD
QB = 2 * SEG
HALO = LEFT * SEG
KB = QB + HALO
LINE = KB + QB
FIRST = QB - (SEG - 1)
UNSEEN = -1e30
GROUPS = 3
F32 = jnp.float32
BF16 = jnp.bfloat16


def attention_kernel(
    lim_ref, qh_ref, qt_ref, kh_ref, kt_ref, kp_ref, vh_ref, vt_ref, vp_ref, do_ref, line_ref,
    dq_ref, dkh_ref, dkt_ref, dvh_ref, dvt_ref, back_ref, lg_ref,
    kext, vext, ktr, qall, dkx, dvx, bias, dsum,
):
    rows = do_ref.shape[0]
    head_rows = rows - HALO
    scale = HEAD ** -0.5
    kext[:HALO, :] = kp_ref[...]
    kext[HALO : HALO + head_rows, :] = kh_ref[...]
    kext[HALO + head_rows :, :] = kt_ref[...]
    vext[:HALO, :] = vp_ref[...]
    vext[HALO : HALO + head_rows, :] = vh_ref[...]
    vext[HALO + head_rows :, :] = vt_ref[...]
    qall[:head_rows, :] = qh_ref[...]
    qall[head_rows:, :] = qt_ref[...]
    ktr[...] = kext[...].T
    dkx[...] = jnp.zeros_like(dkx)
    dvx[...] = jnp.zeros_like(dvx)
    line = line_ref[0]
    ki = lax.broadcasted_iota(jnp.int32, (QB, QB), 0)
    qi = lax.broadcasted_iota(jnp.int32, (QB, QB), 1)
    blocks = KB // QB
    for h in range(2):
        for j in range(blocks):
            at = KB - QB - QB * j
            window = jnp.broadcast_to(line[h : h + 1, at : at + 2 * QB], (QB, 2 * QB))
            skewed = pltpu.roll(window, QB, 1, stride=1, stride_axis=0)[:, :QB]
            k_seg = (ki + QB * j) // SEG
            q_seg = qi // SEG
            seen = (k_seg >= q_seg) & (k_seg <= q_seg + LEFT)
            bias[QB * j : QB * (j + 1), QB * h : QB * (h + 1)] = jnp.where(seen, skewed, UNSEEN)
    low = lax.broadcasted_iota(jnp.int32, (QB, PAIR), 1) < HEAD
    zero = jnp.zeros((QB, PAIR), BF16)
    last_dims = (((1,), (1,)), ((), ()))
    lim = lim_ref[0]
    for b in range(rows // QB):
        q_rows = pl.ds(QB * b, QB)
        k_rows = pl.ds(QB * b, KB)
        q = qall[q_rows, :] * jnp.bfloat16(scale)
        d = do_ref[q_rows, :]
        q_two = jnp.concatenate([jnp.where(low, q, zero), jnp.where(low, zero, q)], axis=0)
        d_two = jnp.concatenate([jnp.where(low, d, zero), jnp.where(low, zero, d)], axis=0)
        s = lax.dot_general(kext[k_rows, :], q_two, last_dims, preferred_element_type=F32)
        s = s + bias[...]
        if QB * b < HALO:
            row = lax.broadcasted_iota(jnp.int32, s.shape, 0) + QB * b
            s = jnp.where(row < lim, UNSEEN, s)
        top = jnp.max(s, axis=0, keepdims=True)
        p = jnp.exp(s - top)
        prob = p * (1.0 / jnp.sum(p, axis=0, keepdims=True))
        prob_low = prob.astype(BF16)
        grad_prob = lax.dot_general(vext[k_rows, :], d_two, last_dims, preferred_element_type=F32)
        delta = jnp.sum(prob_low.astype(F32) * grad_prob, axis=0, keepdims=True)
        ds = prob * (grad_prob - delta)
        ds_low = ds.astype(BF16)
        dvx[k_rows, :] += jnp.dot(prob_low, d_two, preferred_element_type=F32)
        dkx[k_rows, :] += jnp.dot(ds_low, q_two, preferred_element_type=F32)
        dq = jnp.dot(ktr[:, k_rows], ds_low, preferred_element_type=F32)
        dq = jnp.concatenate([dq[:HEAD, :QB], dq[HEAD:, QB:]], axis=0) * scale
        dq_ref[q_rows, :] = dq.T.astype(BF16)
        if b == 0:
            dsum[...] = ds
        else:
            dsum[...] += ds
    dkh_ref[...] = dkx[HALO : HALO + head_rows, :].astype(BF16)
    dkt_ref[...] = dkx[HALO + head_rows :, :]
    dvh_ref[...] = dvx[HALO : HALO + head_rows, :].astype(BF16)
    dvt_ref[...] = dvx[HALO + head_rows :, :]
    back_ref[0] = dkx[:HALO, :].astype(BF16)
    back_ref[1] = dvx[:HALO, :].astype(BF16)
    flip = (ki + qi == QB - 1).astype(F32)
    pad = jnp.zeros((QB, QB), F32)
    for h in range(2):
        sums = []
        for j in range(blocks):
            a = dsum[QB * j : QB * (j + 1), QB * h : QB * (h + 1)]
            a = jnp.dot(flip, a, precision=lax.Precision.HIGHEST, preferred_element_type=F32)
            y = pltpu.roll(jnp.concatenate([a, pad], axis=1), 1, 1, stride=1, stride_axis=0)
            sums.append(jnp.sum(y, axis=0, keepdims=True))
        pieces = []
        for c in range(blocks + 1):
            parts = []
            if c < blocks:
                parts.append(sums[blocks - 1 - c][:, :QB])
            if c > 0:
                parts.append(sums[blocks - c][:, QB:])
            pieces.append(sum(parts[1:], parts[0]))
        lg_ref[0, h : h + 1, :] = jnp.concatenate(pieces, axis=1)


def attention(lim, q, k, v, prior, d_out, line, first_pair, pairs):
    rows = d_out.shape[0]
    cols = d_out.shape[1]
    head_rows = rows - HALO
    width = pairs * PAIR

    def arg(height, skip=0):
        return pl.BlockSpec((height, PAIR), lambda i: (0, i + skip))

    def out(height, dtype):
        return jax.ShapeDtypeStruct((height, width), dtype)

    both = [arg(head_rows, first_pair), arg(HALO, first_pair)]
    mac = 2 * rows * KB * PAIR * 2 * pairs * 5 // 2
    return pl.pallas_call(
        attention_kernel,
        grid=(pairs,),
        in_specs=[pl.BlockSpec(memory_space=pltpu.SMEM)]
        + both
        + both
        + [arg(HALO, first_pair)]
        + both
        + [arg(HALO, first_pair + cols // PAIR), arg(rows, first_pair)]
        + [pl.BlockSpec((1, 2, LINE), lambda i: (i + first_pair, 0, 0))],
        out_specs=[
            arg(rows),
            arg(head_rows),
            arg(HALO),
            arg(head_rows),
            arg(HALO),
            pl.BlockSpec((2, HALO, PAIR), lambda i: (0, 0, i)),
            pl.BlockSpec((1, 2, LINE), lambda i: (i, 0, 0)),
        ],
        out_shape=[
            out(rows, BF16),
            out(head_rows, BF16),
            out(HALO, F32),
            out(head_rows, BF16),
            out(HALO, F32),
            jax.ShapeDtypeStruct((2, HALO, width), BF16),
            jax.ShapeDtypeStruct((pairs, 2, LINE), F32),
        ],
        scratch_shapes=[
            pltpu.VMEM((rows + HALO, PAIR), BF16),
            pltpu.VMEM((rows + HALO, PAIR), BF16),
            pltpu.VMEM((PAIR, rows + HALO), BF16),
            pltpu.VMEM((rows, PAIR), BF16),
            pltpu.VMEM((rows + HALO, PAIR), F32),
            pltpu.VMEM((rows + HALO, PAIR), F32),
            pltpu.VMEM((KB, 2 * QB), F32),
            pltpu.VMEM((KB, 2 * QB), F32),
        ],
        cost_estimate=pl.CostEstimate(flops=mac * 8, bytes_accessed=rows * width * 20, transcendentals=0),
    )(lim, q[0], q[1], k[0], k[1], prior, v[0], v[1], prior, d_out, line)


def bias_line(rel_bias):
    after = LINE - FIRST - rel_bias.shape[0]
    line = jnp.pad(rel_bias.T, ((0, 0), (FIRST, after)), mode="edge")
    return line.reshape(-1, 2, LINE)


def bias_line_back(line, count):
    line = line.reshape(-1, LINE)
    start = jnp.sum(line[:, : FIRST + 1], axis=1, keepdims=True)
    end = jnp.sum(line[:, FIRST + count - 1 :], axis=1, keepdims=True)
    return jnp.concatenate([start, line[:, FIRST + 1 : FIRST + count - 1], end], axis=1)


def shifted(block, axis, by):
    n = lax.axis_size(axis)
    return lax.ppermute(block, axis, [(i, (i + by) % n) for i in range(n)])


def crossed(block, axis, bits):
    n = lax.axis_size(axis)
    return lax.ppermute(block, axis, [(i, i ^ bits) for i in range(n)])


def passed_along(block, axis, distance):
    devices = range(lax.axis_size(axis))
    return lax.ppermute(block, axis, [(i - distance, i) for i in devices if i - distance in devices])


def all_features(block):
    n = lax.axis_size("tp")
    own = lax.axis_index("tp")
    width = block.shape[1]
    whole = jnp.zeros((block.shape[0], width * n), block.dtype)
    whole = lax.dynamic_update_slice(whole, block, (0, own * width))
    for step in range(1, n):
        whole = lax.dynamic_update_slice(
            whole, shifted(block, "tp", step), (0, (own - step) % n * width)
        )
    return whole


def dot(a, b):
    return jnp.dot(a, b, preferred_element_type=F32)


def local(inputs, w_query, w_key, w_value, rel_bias, d_out):
    n_sp = lax.axis_size("sp")
    n_tp = lax.axis_size("tp")
    sp = lax.axis_index("sp")
    tp = lax.axis_index("tp")
    rows, d_here = inputs.shape
    cols = d_out.shape[1]
    head_rows = rows - HALO
    depth = d_here * n_tp
    tail = all_features(inputs[head_rows:])
    head = all_features(inputs[:head_rows])
    k_tail = dot(tail, w_key).astype(BF16)
    v_tail = dot(tail, w_value).astype(BF16)
    prior = passed_along(jnp.concatenate([k_tail, v_tail], axis=1), "sp", 1)
    q = (dot(head, w_query).astype(BF16), dot(tail, w_query).astype(BF16))
    k = (dot(head, w_key).astype(BF16), k_tail)
    v = (dot(head, w_value).astype(BF16), v_tail)

    ring = n_sp // 4
    share = depth // n_sp
    z = sp // 4
    y = sp // 2 % 2
    c = sp % 2
    flipped = jnp.concatenate([head, tail], axis=0).T.reshape(ring, 2, 2, share, rows)

    def of_quad(which):
        return jnp.concatenate(
            [
                lax.dynamic_slice(flipped, (z ^ j, which, 0, 0, 0), (1, 1, 2, share, rows))[:, 0]
                for j in range(ring)
            ],
            axis=0,
        )

    pair_x = jnp.concatenate([of_quad(y), crossed(of_quad(1 - y), "sp", 2)], axis=3)
    mine = lax.dynamic_slice(pair_x, (0, c, 0, 0), (ring, 1, share, 2 * rows))[:, 0]
    other = lax.dynamic_slice(pair_x, (0, 1 - c, 0, 0), (ring, 1, share, 2 * rows))[:, 0]
    other = crossed(other, "sp", 1)
    mine = mine.reshape(ring * share, 2 * rows)
    other = other.reshape(ring * share, 2 * rows)

    lim = jnp.where(sp == 0, HALO, 0).astype(jnp.int32).reshape(1)
    line = bias_line(rel_bias)
    pairs = cols // PAIR
    groups = GROUPS if pairs % GROUPS == 0 else 1
    each = pairs // groups
    lines = []
    grads = []
    w_grads = []
    for g in range(groups):
        dq, dk_head, dk_tail, dv_head, dv_tail, back, lg = attention(
            lim, q, k, v, prior, d_out, line, g * each, each
        )
        lines.append(lg)
        back = passed_along(back, "sp", -1).astype(F32)
        dk = jnp.concatenate([dk_head, (dk_tail + back[0]).astype(BF16)], axis=0)
        dv = jnp.concatenate([dv_head, (dv_tail + back[1]).astype(BF16)], axis=0)
        grads.append((dq, dk, dv))
        packed = jnp.concatenate([dq, dk, dv], axis=1)
        packed = jnp.concatenate([packed, crossed(packed, "sp", 2)], axis=0)
        packed_other = crossed(packed, "sp", 1)
        partial = (dot(mine, packed) + dot(other, packed_other)).astype(BF16)
        total = partial[:share].astype(F32)
        for j in range(1, ring):
            total = total + crossed(partial[j * share : (j + 1) * share], "sp", 4 * j).astype(F32)
        w_grads.append(total)
    width = each * PAIR
    grad_w = [
        jnp.concatenate([t[:, i * width : (i + 1) * width] for t in w_grads], axis=1)
        for i in range(3)
    ]

    last_dims = (((1,), (1,)), ((), ()))
    partial_x = None
    for i, w in enumerate((w_query, w_key, w_value)):
        grad = jnp.concatenate([g[i] for g in grads], axis=1)
        term = lax.dot_general(grad, w, last_dims, preferred_element_type=F32)
        partial_x = term if partial_x is None else partial_x + term
    partial_x = partial_x.astype(BF16)
    total_x = lax.dynamic_slice(partial_x, (0, tp * d_here), (rows, d_here)).astype(F32)
    for step in range(1, n_tp):
        piece = lax.dynamic_slice(partial_x, (0, (tp + step) % n_tp * d_here), (rows, d_here))
        total_x = total_x + shifted(piece, "tp", step).astype(F32)
    grad_inputs = total_x.astype(BF16)

    grad_bias = bias_line_back(jnp.concatenate(lines, axis=0), rel_bias.shape[0])
    bit = 1
    while bit < n_sp:
        grad_bias = grad_bias + crossed(grad_bias, "sp", bit)
        bit *= 2
    return (grad_inputs, grad_w[0], grad_w[1], grad_w[2], grad_bias.T)


def solution(mesh):
    placed = (
        P("sp", "tp"),
        P(None, "tp"),
        P(None, "tp"),
        P(None, "tp"),
        P(None, "tp"),
        P("sp", "tp"),
    )
    return jax.shard_map(
        local,
        mesh=mesh,
        in_specs=placed,
        out_specs=(P("sp", "tp"), P("sp", "tp"), P("sp", "tp"), P("sp", "tp"), P(None, "tp")),
        check_vma=False,
    )
```
